32 devices in a mesh: gr: 2 (over core), fs: 8 (over z, y), tp: 2 (over x).
Axes of the slice: x: 2, y: 2, z: 4, core: 2. Of those that a mesh axis runs over, the one named last changes fastest.
Arguments:
- prompt: bfloat16 [5120, 2048], P(('gr', 'fs'), 'tp'), may hold values from -6 to 6
- norm_gain: float32 [2048], P(('gr', 'fs')), may hold values from 0.1 to 1.9
- gate_weight: float32 [32, 2048, 2048], P(None, ('gr', 'fs'), 'tp'), may hold values from -0.125 to 0.125
- up_weight: float32 [32, 2048, 2048], P(None, ('gr', 'fs'), 'tp'), may hold values from -0.125 to 0.125
- down_weight: float32 [32, 2048, 2048], P(None, ('gr', 'fs'), 'tp'), may hold values from -0.125 to 0.125
- routes: int32 [5120, 2], P(('gr', 'fs')), may hold values from 0 to 31, as said below
- route_weight: float32 [5120, 2], P(('gr', 'fs')), may hold values from 0.2 to 1
Outputs:
- gate_new: bfloat16 [32, 2048, 2048], P('fs', None, 'tp')
- up_new: bfloat16 [32, 2048, 2048], P('fs', None, 'tp')
- down_new: bfloat16 [32, 2048, 2048], P('fs', 'tp')
- mixed: bfloat16 [5120, 2048], P(('gr', 'fs'), 'tp')
The draws below stay inside these ranges and needn't reach their ends.
Inputs may be any that keep to these rules, and one draw needn't show every extreme that they name: `routes`: each row names two different experts of the same group; expert e belongs to group e // 8. Among the 320 rows of one index of gr and fs no expert is named more than 30 times, and in every draw every expert of one group is named exactly 30 times by the rows of every index.
All inputs are finite; a program needn't handle non-finite values.
Results may differ from the reference program's by a relative error of at most 0.015.
Values may be sent and summed in bfloat16 or wider, within the bound.
A program may use at most 256 MiB of HBM per device.

```python
import jax
import jax.numpy as jnp
from jax import lax

D = 2048
FF = 2048
GROUPS = 4
EXP_GROUP = 8
TOK_DEV = 320
EXPERTS = 32
CAP = 30
TOKENS = 5120
N_GR = 2
N_FS = 8
N_TP = 2


def draw_routes(key, part):
    big_group = jax.random.randint(jax.random.fold_in(key, 101), (), 0, GROUPS)
    full = 4 * CAP
    rest = TOK_DEV - full
    spacing = rest // (GROUPS - 1)
    jitter = spacing // 4

    def one_source(source):
        source_key = jax.random.fold_in(key, source)
        key_rank, key_bound, key_shift = jax.random.split(source_key, 3)
        ranking = jax.random.permutation(key_rank, TOK_DEV).astype(jnp.int32)
        inner = jnp.arange(1, GROUPS - 1, dtype=jnp.int32) * rest // (GROUPS - 1)
        inner = inner + jax.random.randint(key_bound, (GROUPS - 2,), -jitter, jitter + 1)
        bounds = jnp.concatenate([jnp.zeros((1,), jnp.int32), inner.astype(jnp.int32)])
        remain = ranking - full
        slot_index = jnp.sum((remain[:, None] >= inner[None, :]).astype(jnp.int32), axis=1)
        in_big = ranking < full
        within = jnp.where(in_big, ranking, remain - bounds[slot_index])
        other = slot_index + (slot_index >= big_group).astype(jnp.int32)
        group_id = jnp.where(in_big, big_group, other)
        shifts = jax.random.randint(key_shift, (GROUPS,), 0, EXP_GROUP)
        offset = shifts[group_id]
        first = (within + offset) % EXP_GROUP
        second = (within + offset + 1 + within // EXP_GROUP % (EXP_GROUP - 1)) % EXP_GROUP
        return jnp.stack([group_id * EXP_GROUP + first, group_id * EXP_GROUP + second], axis=1)
    sources = jnp.arange(N_GR * N_FS, dtype=jnp.int32)
    return jax.vmap(one_source)(sources).reshape(TOKENS, 2).astype(jnp.int32)


def level_of(key, extent, shards, low, top_value):
    gain, own = 1.0, jax.random.fold_in(key, 6)
    for position, shards_of in shards:
        steps = jnp.exp(jax.random.uniform(jax.random.fold_in(own, position), (shards_of,), jnp.float32, low / len(shards), top_value / len(shards)))
        gain = gain * jnp.repeat(steps, extent[position] // shards_of).reshape([-1 if axis == position else 1 for axis in range(len(extent))])
    return gain


def normal_values(rng, shape, width, most, cuts=(), held_as=jnp.bfloat16):
    drawn = jax.random.normal(rng, shape, jnp.float32) * width
    if len(cuts) > 0:
        drawn = level_of(rng, shape, cuts, -0.22, 0.18) * drawn
    return jnp.clip(drawn, min=-most, max=most).astype(held_as)


def setup_inputs(seed: int = 0) -> dict:
    streams_of = jax.random.split(jax.random.key(seed), 8)
    return {
        "prompt": normal_values(streams_of[0], (TOKENS, D), 1.0, 6.0, ((0, 16), (1, 2))),
        "norm_gain": jnp.clip(1.0 + 0.18 * jax.random.normal(streams_of[1], (D,), jnp.float32), 0.1, 1.9),
        "gate_weight": normal_values(streams_of[2], (EXPERTS, D, FF), D ** -0.5, 0.125, ((1, 16), (2, 2)), jnp.float32),
        "up_weight": normal_values(streams_of[3], (EXPERTS, D, FF), D ** -0.5, 0.125, ((1, 16), (2, 2)), jnp.float32),
        "down_weight": normal_values(streams_of[4], (EXPERTS, FF, D), FF ** -0.5, 0.125, ((1, 16), (2, 2)), jnp.float32),
        "routes": draw_routes(jax.random.fold_in(streams_of[7], 71), 0),
        "route_weight": jnp.clip(0.2 + 0.8 * jax.random.uniform(streams_of[6], (TOKENS, 2), jnp.float32) ** level_of(streams_of[6], (TOKENS, 2), ((0, 16),), -0.2, 0.2), 0.2, 1.0),
    }


def reference(prompt, norm_gain, gate_weight, up_weight, down_weight, routes, route_weight):
    gate_new = (gate_weight * norm_gain[None, :, None]).astype(jnp.bfloat16)
    up_new = (up_weight * norm_gain[None, :, None]).astype(jnp.bfloat16)
    down_new = down_weight.astype(jnp.bfloat16)
    values = prompt.astype(jnp.float32)
    normed = (values * lax.rsqrt(lax.optimization_barrier(jnp.mean(values * values, axis=-1, keepdims=True)) + 1e-06)).astype(jnp.bfloat16)
    picks_flat = routes.reshape(-1)
    total = picks_flat.shape[0]
    most = N_GR * N_FS * CAP
    normed_pad = jnp.concatenate([normed, jnp.zeros((1, D), jnp.bfloat16)], axis=0)
    weight_pad = jnp.concatenate([route_weight.reshape(-1), jnp.zeros((1,), jnp.float32)], axis=0)

    def one_expert(accum, expert):
        chosen = jnp.nonzero(picks_flat == expert, size=most, fill_value=total)[0].astype(jnp.int32)
        tok_rows = (chosen // 2).astype(jnp.int32)
        arrived = normed_pad[tok_rows]
        gate_pre = jnp.dot(arrived, gate_new[expert], preferred_element_type=jnp.float32)
        up_pre = jnp.dot(arrived, up_new[expert], preferred_element_type=jnp.float32)
        hidden = (jax.nn.silu(gate_pre) * up_pre).astype(jnp.bfloat16)
        blocks = hidden.reshape(most, N_TP, FF // N_TP).astype(jnp.float32)
        down_blocks = down_new[expert].reshape(N_TP, FF // N_TP, D).astype(jnp.float32)
        partial_value = jnp.einsum('rkh,khd->rkd', blocks, down_blocks).astype(jnp.bfloat16)
        partial_value = lax.optimization_barrier(partial_value).astype(jnp.float32)
        expert_out = lax.optimization_barrier(jnp.sum(partial_value, axis=1)).astype(jnp.bfloat16)
        expert_out = lax.optimization_barrier(expert_out).astype(jnp.float32)
        accum = accum.at[tok_rows].add(expert_out * weight_pad[chosen][:, None])
        return (accum, None)
    start = jnp.zeros((TOKENS + 1, D), jnp.float32)
    accum, _ = lax.scan(one_expert, start, jnp.arange(EXPERTS, dtype=jnp.int32))
    mixed = accum[:TOKENS].astype(jnp.bfloat16)
    return (gate_new, up_new, down_new, mixed)
```

```python
import functools

import jax
import jax.numpy as jnp
from jax import lax
from jax.experimental import pallas as pl
from jax.experimental.pallas import tpu as pltpu
from jax.sharding import PartitionSpec as P

CAP = 30
EXP_GROUP = 8
SLOT = -(-CAP // 16) * 16
GROUP_ROWS = -(-(EXP_GROUP * CAP // 2) // 128) * 128
MESH = pl.DeviceIdType.MESH
F32, BF16 = jnp.float32, jnp.bfloat16


def remote(src, dst, send, recv, device):
    copy = pltpu.make_async_remote_copy(
        src_ref=src, dst_ref=dst, send_sem=send, recv_sem=recv, device_id=device, device_id_type=MESH
    )
    copy.start()


def settle(ref, sem):
    pltpu.make_async_copy(ref, ref, sem).wait()


def loop(low, high, step):
    lax.fori_loop(low, high, lambda index, carry: (step(index), carry)[1], 0)


def span(index, size):
    return pl.ds(pl.multiple_of(index * size, size), size)


def greet(barrier, device):
    pl.semaphore_signal(barrier, inc=1, device_id=device, device_id_type=MESH)


def iota(shape, axis):
    return lax.broadcasted_iota(jnp.int32, shape, axis)


def dot(a, b):
    return jnp.dot(a, b, preferred_element_type=F32)


IN_SLOTS = 3
OUT_SLOTS = 2
EARLY = 4


def serve_kernel(
    sizes, gate, up, down, gain, prompt, routes_lane, routes_sub, weight_sub,
    gate_land, up_land, down_land, cast, mixed,
    stage_in, stage_out, prompt_pad, tok_own, meta_own, tok_land, meta_land,
    rows, pick, w_vmem, down_vmem, hidden, part, got, summed, ret,
    in_sem, out_sem, w_send, w_recv, tok_send, tok_recv, share_send, share_recv,
    meta_send, meta_recv, twin_send, twin_recv, load_sem, x_send, x_recv, z_send, z_recv,
):
    n_gr, n_fs, n_tp = sizes
    gr, fs, tp = lax.axis_index("gr"), lax.axis_index("fs"), lax.axis_index("tp")
    experts, blk, wide = gate.shape
    per = experts // n_fs
    groups = experts // EXP_GROUP
    reach = EXP_GROUP // per
    seats = n_fs // reach
    full = wide * n_tp
    toks, pad = prompt.shape[0], prompt_pad.shape[0]
    per_tp = n_gr * n_fs // n_tp
    row = gr * n_fs + fs
    owner = row // per_tp
    home = tp * per_tp // n_fs
    ring = n_fs * n_tp
    steps = per * n_fs
    weights = (gate, up, down)
    member = fs % reach
    my_group = fs // reach

    def offset(k):
        return (k + n_fs // 2 - 1) % (n_fs - 1) + 1

    def target_of(step):
        k = step % n_fs
        return jnp.where(k < n_fs - 1, (fs + offset(k)) % n_fs, fs)

    def load(step):
        e = target_of(step) * per + step // n_fs
        slot = step % IN_SLOTS
        return [
            pltpu.make_async_copy(ref.at[e], stage_in.at[slot, w], in_sem.at[slot, w])
            for w, ref in enumerate(weights)
        ]

    def start_load(step):
        for copy in load(step):
            copy.start()

    for step in range(min(IN_SLOTS, steps)):
        start_load(step)

    barrier = pltpu.get_barrier_semaphore()

    def greet_plane(k):
        other = (fs * n_tp + tp + k) % ring
        greet(barrier, (gr, other // n_tp, other % n_tp))

    loop(1, ring, greet_plane)
    loop(1, n_gr, lambda k: greet(barrier, ((gr + k) % n_gr, fs, tp)))
    pl.semaphore_wait(barrier, ring + n_gr - 2)

    def own_row(out, x, index):
        return out.at[x, span(index, blk), :]

    def down_place(x, index, t):
        return down_land.at[x, span(index, blk), span(t, wide)]

    scale = gain[...]

    def put(step):
        x, f, slot = step // n_fs, target_of(step), step % OUT_SLOTS
        e = f * per + x

        @pl.when(f != fs)
        def _():
            for w in range(3):
                pltpu.make_async_copy(stage_out.at[slot, w], cast.at[w, e], out_sem.at[slot, w]).start()

        @pl.when(f == fs)
        def _():
            for w, out in enumerate((gate_land, up_land)):
                pltpu.make_async_copy(stage_out.at[slot, w], own_row(out, x, row), out_sem.at[slot, w]).start()

            @pl.when(owner == tp)
            def _():
                place = down_place(x, row - owner * per_tp, tp)
                pltpu.make_async_copy(stage_out.at[slot, 2], place, out_sem.at[slot, 2]).start()

            @pl.when(owner != tp)
            def _():
                pltpu.make_async_copy(stage_out.at[slot, 2], cast.at[2, e], out_sem.at[slot, 2]).start()

    def dispatch(step):
        x, f, slot = step // n_fs, target_of(step), step % OUT_SLOTS
        e = f * per + x
        for w in range(3):
            settle(stage_out.at[slot, w], out_sem.at[slot, w])

        @pl.when(f != fs)
        def _():
            for w, out in enumerate((gate_land, up_land)):
                remote(cast.at[w, e], own_row(out, x, row), w_send.at[w], w_recv.at[w, x, fs], (gr, f, tp))
            place = down_place(x, row - owner * per_tp, tp)
            remote(cast.at[2, e], place, w_send.at[2], w_recv.at[2, x, fs], (gr, f, owner))

        @pl.when((f == fs) & (owner != tp))
        def _():
            place = down_place(x, row - owner * per_tp, tp)
            remote(cast.at[2, e], place, w_send.at[2], w_recv.at[2, x, fs], (gr, fs, owner))

    def cast_step(step):
        slot, out_slot = step % IN_SLOTS, step % OUT_SLOTS
        for copy in load(step):
            copy.wait()
        stage_out[out_slot, 0] = (stage_in[slot, 0] * scale).astype(BF16)
        stage_out[out_slot, 1] = (stage_in[slot, 1] * scale).astype(BF16)
        stage_out[out_slot, 2] = stage_in[slot, 2].astype(BF16)
        put(step)

        @pl.when(step > 0)
        def _():
            dispatch(step - 1)

        @pl.when(step + IN_SLOTS < steps)
        def _():
            start_load(step + IN_SLOTS)

    early = min(EARLY, steps)
    loop(0, early, cast_step)

    prompt_pad[pl.ds(0, toks), :] = prompt[...]
    if pad > toks:
        prompt_pad[pl.ds(toks, pad - toks), :] = jnp.zeros((pad - toks, wide), BF16)
    first, second = routes_lane[0:1, :], routes_lane[1:2, :]
    group_pad = -(-groups // 8) * 8
    low = iota((group_pad, pad), 0) * EXP_GROUP
    in_group = (first >= low) & (first < low + EXP_GROUP)
    expert_ids = iota((experts, pad), 0)
    named = (first == expert_ids) | (second == expert_ids)
    before = jnp.where(iota((pad, pad), 0) < iota((pad, pad), 1), 1.0, 0.0).astype(BF16)
    place_in = dot(jnp.where(in_group, 1.0, 0.0).astype(BF16), before).astype(jnp.int32)
    slot_in = dot(jnp.where(named, 1.0, 0.0).astype(BF16), before)
    slot_in = jnp.where(named, slot_in + 1.0, 0.0).astype(BF16)
    place_in = jnp.where(in_group, place_in, -1)
    for g in range(groups):
        pack = jnp.where(iota((GROUP_ROWS, pad), 0) == place_in[g : g + 1, :], 1.0, 0.0).astype(BF16)
        tok_own[g] = dot(pack, prompt_pad[...]).astype(BF16)
        meta_own[g] = lax.dot_general(
            slot_in[g * EXP_GROUP : (g + 1) * EXP_GROUP, :], pack,
            (((1,), (1,)), ((), ())), preferred_element_type=F32,
        )

    def send_tok(k):
        g = (my_group + k) % groups
        f = g * reach + member
        remote(tok_own.at[g], tok_land.at[tp, fs], tok_send, tok_recv.at[fs // reach], (gr, f, tp))

    loop(1, groups, send_tok)
    tok_land[tp, fs] = tok_own[my_group]
    meta_land[fs] = meta_own[my_group]

    def send_meta(k):
        f = (fs + k) % n_fs
        remote(meta_own.at[f // reach], meta_land.at[fs], meta_send, meta_recv, (gr, f, tp))

    loop(1, n_fs, send_meta)

    loop(early, steps, cast_step)
    dispatch(jnp.int32(steps - 1))

    def share_tok(q):
        seat = (my_group + q) % seats
        source = seat * reach + member
        place = tok_land.at[tp, source]

        @pl.when(source != fs)
        def _():
            settle(place, tok_recv.at[seat])

        def forward(j):
            seat_of = (member * n_tp + tp + j) % (reach * n_tp)
            f, t = my_group * reach + seat_of // n_tp, seat_of % n_tp
            remote(place, place, share_send, share_recv.at[tp], (gr, f, t))

        loop(1, reach * n_tp, forward)

    loop(0, seats, share_tok)

    pick_r0, pick_r1 = routes_sub[:, 0:1], routes_sub[:, 1:2]
    lane_pad = -(-experts // 128) * 128
    lanes = iota((pad, lane_pad), 1)
    named_sub = (pick_r0 == lanes) | (pick_r1 == lanes)
    before_sub = jnp.where(iota((pad, pad), 1) < iota((pad, pad), 0), 1.0, 0.0).astype(BF16)
    slots_sub = dot(before_sub, jnp.where(named_sub, 1.0, 0.0).astype(BF16))
    for j, r in enumerate((pick_r0, pick_r1)):
        slot_of = jnp.sum(jnp.where(r == lanes, slots_sub, 0.0), axis=1, keepdims=True).astype(jnp.int32)
        spot = r * SLOT + slot_of
        pick[j] = jnp.where(iota((pad, experts * SLOT), 1) == spot, 1.0, 0.0).astype(BF16)

    for j in range(n_tp):
        t = (tp + j) % n_tp
        if j > 0:
            settle(tok_land.at[t], share_recv.at[t])
        elif reach > 1:
            settle(tok_land.at[t, pl.ds(0, n_fs - seats)], share_recv.at[t])
    settle(meta_land.at[pl.ds(0, n_fs - 1)], meta_recv)

    def make_rows(source):
        total = jnp.zeros((GROUP_ROWS, 1), F32)
        for t in range(n_tp):
            values = tok_land[t, source].astype(F32)
            total = total + jnp.sum(values * values, axis=1, keepdims=True)
        factor = lax.rsqrt(total / full + 1e-06)
        for t in range(n_tp):
            normed = (tok_land[t, source].astype(F32) * factor).astype(BF16)
            for x in range(per):
                line = meta_land[source, pl.ds(member * per + x, 1), :]
                choose = jnp.where(
                    iota((SLOT, GROUP_ROWS), 0) + 1 == line.astype(jnp.int32), 1.0, 0.0
                ).astype(BF16)
                rows[x, span(source, SLOT), t * wide : (t + 1) * wide] = dot(choose, normed).astype(BF16)

    loop(0, n_fs, make_rows)

    tile = min(wide, 256)
    tile_full = min(full, 256)

    def serve(x):
        def twins(k):
            source = jnp.where(k > 0, (fs + n_fs - offset(k - 1)) % n_fs, fs)
            index = gr * n_fs + source

            @pl.when(source != fs)
            def _():
                for w, out in enumerate((gate_land, up_land)):
                    settle(own_row(out, x, index), w_recv.at[w, x, source])

            for w, out in enumerate((gate_land, up_land)):
                place = own_row(out, x, index)
                for j in range(1, n_gr):
                    g = (gr + j) % n_gr
                    remote(place, place, twin_send.at[w, g], twin_recv.at[w, x, gr], (g, fs, tp))

            @pl.when(index // per_tp == tp)
            def _():
                place = own_row(down_land, x, index - tp * per_tp)

                @pl.when(source != fs)
                def _():
                    settle(place, w_recv.at[2, x, source])

                @pl.when(source == fs)
                def _():
                    if n_tp > 1:
                        settle(down_land.at[x, span(index - tp * per_tp, blk), pl.ds(0, (n_tp - 1) * wide)], w_recv.at[2, x, fs])

                for j in range(1, n_gr):
                    g = (gr + j) % n_gr
                    remote(place, place, twin_send.at[2, g], twin_recv.at[2, x, gr], (g, fs, tp))

        loop(0, n_fs, twins)
        for j in range(1, n_gr):
            g = (gr + j) % n_gr
            for w, out in enumerate((gate_land, up_land)):
                settle(out.at[x, span(g, n_fs * blk), :], twin_recv.at[w, x, g])

        @pl.when(home != gr)
        def _():
            settle(down_land.at[x], twin_recv.at[2, x, home])

        loads = [
            pltpu.make_async_copy(gate_land.at[x], w_vmem.at[0], load_sem.at[0]),
            pltpu.make_async_copy(up_land.at[x], w_vmem.at[1], load_sem.at[1]),
            pltpu.make_async_copy(down_land.at[x], down_vmem, load_sem.at[2]),
        ]
        for copy in loads:
            copy.start()
        loads[0].wait()
        loads[1].wait()

        def hide(c):
            cut = span(c, tile)
            gate_pre = dot(rows[x], w_vmem[0, :, cut])
            up_pre = dot(rows[x], w_vmem[1, :, cut])
            hidden[:, cut] = (jax.nn.silu(gate_pre) * up_pre).astype(BF16)

        loop(0, wide // tile, hide)
        loads[2].wait()

        def lower(c):
            cut = span(c, tile_full)
            part[x, :, cut] = dot(hidden[...], down_vmem[:, cut]).astype(BF16)

        loop(0, full // tile_full, lower)
        for j in range(1, n_tp):
            t = (tp + j) % n_tp
            remote(part.at[x, :, span(t, wide)], got.at[tp, x], x_send.at[t], x_recv.at[tp, x], (gr, fs, t))
        for j in range(1, n_tp):
            t = (tp + j) % n_tp
            settle(got.at[t, x], x_recv.at[t, x])

        def add(f):
            total = part[x, span(f, SLOT), span(tp, wide)].astype(F32)
            for j in range(1, n_tp):
                total = total + got[(tp + j) % n_tp, x, span(f, SLOT), :].astype(F32)
            summed[x, span(f, SLOT), :] = total.astype(BF16)

        loop(0, n_fs, add)

        def back(k):
            f = (fs + offset(k)) % n_fs
            remote(summed.at[x, span(f, SLOT), :], ret.at[span(fs * per + x, SLOT), :], z_send, z_recv, (gr, f, tp))

        loop(0, n_fs - 1, back)
        ret[span(fs * per + x, SLOT), :] = summed[x, span(fs, SLOT), :]

    loop(0, per, serve)

    settle(ret.at[pl.ds(0, (n_fs - 1) * per * SLOT)], z_recv)

    def mix(c):
        cut = span(c, tile)
        out0 = dot(pick[0], ret[:, cut])
        out1 = dot(pick[1], ret[:, cut])
        total = weight_sub[:, 0:1] * out0 + weight_sub[:, 1:2] * out1
        mixed[:, cut] = total[0:toks].astype(BF16)

    loop(0, wide // tile, mix)

    settle(tok_own.at[pl.ds(0, groups - 1)], tok_send)
    settle(meta_land.at[pl.ds(0, n_fs - 1)], meta_send)

    def drain_share(q):
        for _ in range(reach * n_tp - 1):
            settle(tok_land.at[0, pl.ds(0, seats)], share_send)

    loop(0, 1, drain_share)
    for w in range(2):
        settle(cast.at[w, pl.ds(0, (n_fs - 1) * per)], w_send.at[w])

    @pl.when(owner == tp)
    def _():
        settle(cast.at[2, pl.ds(0, (n_fs - 1) * per)], w_send.at[2])

    @pl.when(owner != tp)
    def _():
        settle(cast.at[2], w_send.at[2])

    for j in range(1, n_gr):
        g = (gr + j) % n_gr
        for w, out in enumerate((gate_land, up_land)):
            settle(out.at[:, span(gr, n_fs * blk), :], twin_send.at[w, g])

        @pl.when(home == gr)
        def _():
            settle(down_land, twin_send.at[2, g])

    for j in range(1, n_tp):
        t = (tp + j) % n_tp
        settle(part.at[:, :, span(t, wide)], x_send.at[t])
    settle(ret.at[pl.ds(0, (n_fs - 1) * per * SLOT)], z_send)


def copy_kernel(gate, up, down, gate_out, up_out, down_out):
    gate_out[...] = gate[...]
    up_out[...] = up[...]
    down_out[...] = down[...]


def hand_over(gate, up, down):
    per = gate.shape[0]
    parts = 4

    def spec(array):
        return pl.BlockSpec((1, array.shape[1] // parts, array.shape[2]), lambda x, c: (x, c, 0))

    specs = [spec(gate), spec(up), spec(down)]
    return pl.pallas_call(
        copy_kernel,
        grid=(per, parts),
        out_shape=tuple(jax.ShapeDtypeStruct(a.shape, a.dtype) for a in (gate, up, down)),
        in_specs=specs,
        out_specs=tuple(specs),
        compiler_params=pltpu.CompilerParams(vmem_limit_bytes=60 * 1024 * 1024),
        name="hand_over",
    )(gate, up, down)


def body(sizes, prompt, norm_gain, gate_weight, up_weight, down_weight, routes, route_weight):
    n_gr, n_fs, n_tp = sizes
    tok_count, wide = prompt.shape
    full = wide * n_tp
    experts, blk, _ = gate_weight.shape
    per = experts // n_fs
    groups = experts // EXP_GROUP
    reach = EXP_GROUP // per
    seats = n_fs // reach
    rows_all = n_gr * n_fs * blk
    pad = -(-tok_count // 128) * 128
    routes_sub = jnp.pad(routes, ((0, pad - tok_count), (0, 0)), constant_values=-1)
    routes_lane = jnp.pad(routes_sub.T, ((0, 6), (0, 0)), constant_values=-1)
    weight_sub = jnp.pad(route_weight, ((0, pad - tok_count), (0, 0)))
    any_spec = pl.BlockSpec(memory_space=pl.ANY)
    vmem_spec = pl.BlockSpec(memory_space=pltpu.VMEM)
    dma = pltpu.SemaphoreType.DMA
    held = n_fs * SLOT
    gate_land, up_land, down_land, _, mixed = pl.pallas_call(
        functools.partial(serve_kernel, sizes),
        out_shape=(
            jax.ShapeDtypeStruct((per, rows_all, wide), BF16),
            jax.ShapeDtypeStruct((per, rows_all, wide), BF16),
            jax.ShapeDtypeStruct((per, rows_all // n_tp, full), BF16),
            jax.ShapeDtypeStruct((3, experts, blk, wide), BF16),
            jax.ShapeDtypeStruct((tok_count, wide), BF16),
        ),
        in_specs=[any_spec] * 3 + [vmem_spec] * 5,
        out_specs=(any_spec,) * 4 + (vmem_spec,),
        scratch_shapes=[
            pltpu.VMEM((IN_SLOTS, 3, blk, wide), F32),
            pltpu.VMEM((OUT_SLOTS, 3, blk, wide), BF16),
            pltpu.VMEM((pad, wide), BF16),
            pltpu.VMEM((groups, GROUP_ROWS, wide), BF16),
            pltpu.VMEM((groups, EXP_GROUP, GROUP_ROWS), F32),
            pltpu.VMEM((n_tp, n_fs, GROUP_ROWS, wide), BF16),
            pltpu.VMEM((n_fs, EXP_GROUP, GROUP_ROWS), F32),
            pltpu.VMEM((per, held, full), BF16),
            pltpu.VMEM((2, pad, experts * SLOT), BF16),
            pltpu.VMEM((2, rows_all, wide), BF16),
            pltpu.VMEM((rows_all // n_tp, full), BF16),
            pltpu.VMEM((held, wide), BF16),
            pltpu.VMEM((per, held, full), BF16),
            pltpu.VMEM((n_tp, per, held, wide), BF16),
            pltpu.VMEM((per, held, wide), BF16),
            pltpu.VMEM((experts * SLOT, wide), BF16),
            dma((IN_SLOTS, 3)),
            dma((OUT_SLOTS, 3)),
            dma((3,)),
            dma((3, per, n_fs)),
            dma(()),
            dma((seats,)),
            dma(()),
            dma((n_tp,)),
            dma(()),
            dma(()),
            dma((3, n_gr)),
            dma((3, per, n_gr)),
            dma((3,)),
            dma((n_tp,)),
            dma((n_tp, per)),
            dma(()),
            dma(()),
        ],
        compiler_params=pltpu.CompilerParams(
            collective_id=0, has_side_effects=True, vmem_limit_bytes=58 * 1024 * 1024
        ),
        name="serve",
    )(gate_weight, up_weight, down_weight, norm_gain.reshape(blk, 1), prompt, routes_lane, routes_sub, weight_sub)
    return (*hand_over(gate_land, up_land, down_land), mixed)


def solution(mesh):
    sizes = (mesh.shape["gr"], mesh.shape["fs"], mesh.shape["tp"])
    return jax.shard_map(
        functools.partial(body, sizes),
        mesh=mesh,
        in_specs=(
            P(("gr", "fs"), "tp"),
            P(("gr", "fs")),
            P(None, ("gr", "fs"), "tp"),
            P(None, ("gr", "fs"), "tp"),
            P(None, ("gr", "fs"), "tp"),
            P(("gr", "fs"), None),
            P(("gr", "fs"), None),
        ),
        out_specs=(
            P("fs", None, "tp"),
            P("fs", None, "tp"),
            P("fs", "tp", None),
            P(("gr", "fs"), "tp"),
        ),
        check_vma=False,
    )
```

```python
import functools

import jax
import jax.numpy as jnp
from jax import lax
from jax.experimental import pallas as pl
from jax.experimental.pallas import tpu as pltpu
from jax.sharding import PartitionSpec as P

CAP = 30
EXP_GROUP = 8
SLOT = -(-CAP // 16) * 16
GROUP_ROWS = -(-(EXP_GROUP * CAP // 2) // 128) * 128
MESH = pl.DeviceIdType.MESH
F32, BF16 = jnp.float32, jnp.bfloat16


def remote(src, dst, send, recv, device):
    copy = pltpu.make_async_remote_copy(
        src_ref=src, dst_ref=dst, send_sem=send, recv_sem=recv, device_id=device, device_id_type=MESH
    )
    copy.start()


def settle(ref, sem):
    pltpu.make_async_copy(ref, ref, sem).wait()


def loop(low, high, step):
    lax.fori_loop(low, high, lambda index, carry: (step(index), carry)[1], 0)


def span(index, size):
    return pl.ds(pl.multiple_of(index * size, size), size)


def greet(barrier, device):
    pl.semaphore_signal(barrier, inc=1, device_id=device, device_id_type=MESH)


def iota(shape, axis):
    return lax.broadcasted_iota(jnp.int32, shape, axis)


def dot(a, b):
    return jnp.dot(a, b, preferred_element_type=F32)


IN_SLOTS = 3
OUT_SLOTS = 2
EARLY = 4


def serve_kernel(
    sizes, gate, up, down, gain, prompt, routes, shares,
    gate_land, up_land, down_land, cast, mixed,
    stage_in, stage_out, prompt_pad, routes_pad, shares_pad, tok_own, meta_own, tok_land, meta_land,
    rows, pick, w_vmem, down_vmem, hidden, part, got, summed, ret,
    in_sem, out_sem, w_send, w_recv, tok_send, tok_recv, share_send, share_recv,
    meta_send, meta_recv, twin_send, twin_recv, load_sem, x_send, x_recv, z_send, z_recv, sent_sem,
):
    n_gr, n_fs, n_tp = sizes
    gr, fs, tp = lax.axis_index("gr"), lax.axis_index("fs"), lax.axis_index("tp")
    experts, blk, wide = gate.shape
    per = experts // n_fs
    groups = experts // EXP_GROUP
    reach = EXP_GROUP // per
    seats = n_fs // reach
    full = wide * n_tp
    toks, pad = prompt.shape[0], prompt_pad.shape[0]
    per_tp = n_gr * n_fs // n_tp
    row = gr * n_fs + fs
    owner = row // per_tp
    home = tp * per_tp // n_fs
    ring = n_fs * n_tp
    steps = per * n_fs
    weights = (gate, up, down)
    member = fs % reach
    my_group = fs // reach

    half = n_fs // 2
    base, local = fs // half * half, fs % half
    across = half - base
    blocks = per * (half - 1) // 3
    late = per * half - 2 * blocks
    odd = per * (half - 1) - 3 * blocks

    def plan(step):
        part, rest = step % 5, step - 5 * blocks
        early_far = step // 5 * 2 + jnp.where(part == 3, 1, 0)
        early_near = step // 5 * 3 + jnp.where(part == 4, 2, jnp.where(part == 2, 1, 0))
        in_early = step < 5 * blocks
        is_far = jnp.where(in_early, (part == 0) | (part == 3), rest < late)
        is_own = step >= 5 * blocks + late + odd
        far = jnp.where(in_early, early_far, 2 * blocks + rest)
        near = jnp.where(in_early, early_near, 3 * blocks + rest - late)
        far_x, far_f = far // half, across + (local + far % half) % half
        near_x = near // max(half - 1, 1)
        near_f = base + (local + 1 + near % max(half - 1, 1)) % half
        x = jnp.where(is_own, rest - late - odd, jnp.where(is_far, far_x, near_x))
        return x, jnp.where(is_own, fs, jnp.where(is_far, far_f, near_f))

    def other_to(k):
        return jnp.where(k < half - 1, base + (local + 1 + k) % half, across + (local + k + 1 - half) % half)

    def other_from(k):
        near = base + (local + 2 * half - 1 - k) % half
        return jnp.where(k < half - 1, near, across + (local + 2 * half - 1 - k) % half)

    def load(step):
        x, f = plan(step)
        e = f * per + x
        slot = step % IN_SLOTS
        return [
            pltpu.make_async_copy(ref.at[e], stage_in.at[slot, w], in_sem.at[slot, w])
            for w, ref in enumerate(weights)
        ]

    def start_load(step):
        for copy in load(step):
            copy.start()

    for step in range(min(IN_SLOTS, steps)):
        start_load(step)

    barrier = pltpu.get_barrier_semaphore()

    def greet_plane(k):
        other = (fs * n_tp + tp + k) % ring
        greet(barrier, (gr, other // n_tp, other % n_tp))

    loop(1, ring, greet_plane)
    loop(1, n_gr, lambda k: greet(barrier, ((gr + k) % n_gr, fs, tp)))
    def own_row(out, x, index):
        return out.at[x, span(index, blk), :]

    def down_place(x, index, t):
        return down_land.at[x, span(index, blk), span(t, wide)]

    square = iota((blk, blk), 0) == iota((blk, blk), 1)
    scale = jnp.sum(jnp.where(square, gain[...], 0.0), axis=1, keepdims=True)

    def put(step):
        (x, f), slot = plan(step), step % OUT_SLOTS
        e = f * per + x

        @pl.when(f != fs)
        def _():
            for w in range(3):
                pltpu.make_async_copy(stage_out.at[slot, w], cast.at[w, e], out_sem.at[slot, w]).start()

        @pl.when(f == fs)
        def _():
            for w, out in enumerate((gate_land, up_land)):
                pltpu.make_async_copy(stage_out.at[slot, w], own_row(out, x, row), out_sem.at[slot, w]).start()

            @pl.when(owner == tp)
            def _():
                place = down_place(x, row - owner * per_tp, tp)
                pltpu.make_async_copy(stage_out.at[slot, 2], place, out_sem.at[slot, 2]).start()

            @pl.when(owner != tp)
            def _():
                pltpu.make_async_copy(stage_out.at[slot, 2], cast.at[2, e], out_sem.at[slot, 2]).start()

    def dispatch(step):
        (x, f), slot = plan(step), step % OUT_SLOTS
        e = f * per + x
        for w in range(3):
            settle(stage_out.at[slot, w], out_sem.at[slot, w])

        @pl.when(f != fs)
        def _():
            for w, out in enumerate((gate_land, up_land)):
                remote(cast.at[w, e], own_row(out, x, row), w_send.at[w], w_recv.at[w, x, fs], (gr, f, tp))
            place = down_place(x, row - owner * per_tp, tp)
            remote(cast.at[2, e], place, w_send.at[2], w_recv.at[2, x, fs], (gr, f, owner))

        @pl.when((f == fs) & (owner != tp))
        def _():
            place = down_place(x, row - owner * per_tp, tp)
            remote(cast.at[2, e], place, w_send.at[2], w_recv.at[2, x, fs], (gr, fs, owner))

    def convert(step):
        slot, out_slot = step % IN_SLOTS, step % OUT_SLOTS
        for copy in load(step):
            copy.wait()
        stage_out[out_slot, 0] = (stage_in[slot, 0] * scale).astype(BF16)
        stage_out[out_slot, 1] = (stage_in[slot, 1] * scale).astype(BF16)
        stage_out[out_slot, 2] = stage_in[slot, 2].astype(BF16)
        put(step)

        @pl.when(step + IN_SLOTS < steps)
        def _():
            start_load(step + IN_SLOTS)

    def cast_step(step):
        convert(step)
        dispatch(step - 1)

    early = min(EARLY, steps)
    convert(jnp.int32(0))
    pl.semaphore_wait(barrier, ring + n_gr - 2)
    loop(1, early, cast_step)

    prompt_pad[pl.ds(0, toks), :] = prompt[...]
    if pad > toks:
        prompt_pad[pl.ds(toks, pad - toks), :] = jnp.zeros((pad - toks, wide), BF16)
    routes_pad[...] = jnp.full(routes_pad.shape, -1, jnp.int32)
    routes_pad[0:2, 0:toks] = routes[...]
    shares_pad[...] = jnp.zeros(shares_pad.shape, F32)
    shares_pad[0:2, 0:toks] = shares[...]
    first, second = routes_pad[0:1, :], routes_pad[1:2, :]
    group_pad = -(-groups // 8) * 8
    low = iota((group_pad, pad), 0) * EXP_GROUP
    in_group = (first >= low) & (first < low + EXP_GROUP)
    expert_ids = iota((experts, pad), 0)
    named = (first == expert_ids) | (second == expert_ids)
    before = jnp.where(iota((pad, pad), 0) < iota((pad, pad), 1), 1.0, 0.0).astype(BF16)
    place_in = dot(jnp.where(in_group, 1.0, 0.0).astype(BF16), before).astype(jnp.int32)
    slot_raw = dot(jnp.where(named, 1.0, 0.0).astype(BF16), before)
    slot_in = jnp.where(named, slot_raw + 1.0, 0.0).astype(BF16)
    spots = []
    for r in (first, second):
        slot_of = jnp.sum(jnp.where(r == expert_ids, slot_raw, 0.0), axis=0, keepdims=True)
        spots.append(r * SLOT + slot_of.astype(jnp.int32))
    place_in = jnp.where(in_group, place_in, -1)
    for g in range(groups):
        pack = jnp.where(iota((GROUP_ROWS, pad), 0) == place_in[g : g + 1, :], 1.0, 0.0).astype(BF16)
        tok_own[g] = dot(pack, prompt_pad[...]).astype(BF16)
        meta_own[g] = lax.dot_general(
            slot_in[g * EXP_GROUP : (g + 1) * EXP_GROUP, :], pack,
            (((1,), (1,)), ((), ())), preferred_element_type=F32,
        )

    def send_tok(k):
        g = (my_group + k) % groups
        f = g * reach + member
        remote(tok_own.at[g], tok_land.at[tp, fs], tok_send, tok_recv.at[fs // reach], (gr, f, tp))

    loop(1, groups, send_tok)
    tok_land[tp, fs] = tok_own[my_group]
    meta_land[fs] = meta_own[my_group]

    def send_meta(k):
        f = (fs + k) % n_fs
        remote(meta_own.at[f // reach], meta_land.at[fs], meta_send, meta_recv, (gr, f, tp))

    loop(1, n_fs, send_meta)

    loop(early, steps, cast_step)
    dispatch(jnp.int32(steps - 1))

    def share_tok(q):
        seat = (my_group + q) % seats
        source = seat * reach + member
        place = tok_land.at[tp, source]

        @pl.when(source != fs)
        def _():
            settle(place, tok_recv.at[seat])

        def forward(j):
            seat_of = (member * n_tp + tp + j) % (reach * n_tp)
            f, t = my_group * reach + seat_of // n_tp, seat_of % n_tp
            remote(place, place, share_send, share_recv.at[tp], (gr, f, t))

        loop(1, reach * n_tp, forward)

    loop(0, seats, share_tok)

    def place_picks(e):
        ids = iota((SLOT, pad), 0) + e * SLOT
        weight = jnp.where(ids == spots[0], shares_pad[0:1, :], 0.0) + jnp.where(ids == spots[1], shares_pad[1:2, :], 0.0)
        high = weight.astype(BF16)
        pick[0, span(e, SLOT), :] = high
        pick[1, span(e, SLOT), :] = (weight - high.astype(F32)).astype(BF16)

    loop(0, experts, place_picks)

    for j in range(n_tp):
        t = (tp + j) % n_tp
        if j > 0:
            settle(tok_land.at[t], share_recv.at[t])
        elif reach > 1:
            settle(tok_land.at[t, pl.ds(0, n_fs - seats)], share_recv.at[t])
    settle(meta_land.at[pl.ds(0, n_fs - 1)], meta_recv)

    def make_rows(source):
        total = jnp.zeros((GROUP_ROWS, 1), F32)
        for t in range(n_tp):
            values = tok_land[t, source].astype(F32)
            total = total + jnp.sum(values * values, axis=1, keepdims=True)
        factor = lax.rsqrt(total / full + 1e-06)
        for t in range(n_tp):
            normed = (tok_land[t, source].astype(F32) * factor).astype(BF16)
            for x in range(per):
                line = meta_land[source, pl.ds(member * per + x, 1), :]
                choose = jnp.where(
                    iota((SLOT, GROUP_ROWS), 0) + 1 == line.astype(jnp.int32), 1.0, 0.0
                ).astype(BF16)
                rows[x, span(source, SLOT), t * wide : (t + 1) * wide] = dot(choose, normed).astype(BF16)

    loop(0, n_fs, make_rows)

    tile = min(wide, 256)
    tile_full = min(full, 256)

    def tell_sent():
        for w in range(2):
            settle(cast.at[w, pl.ds(0, (n_fs - 1) * per)], w_send.at[w])

        @pl.when(owner == tp)
        def _():
            settle(cast.at[2, pl.ds(0, (n_fs - 1) * per)], w_send.at[2])

        @pl.when(owner != tp)
        def _():
            settle(cast.at[2], w_send.at[2])

        loop(1, half, lambda k: greet(sent_sem, (gr, base + (local + k) % half, tp)))

    def give_back(x):
        def back(k):
            f = other_to(k)
            remote(summed.at[x, span(f, SLOT), :], ret.at[span(fs * per + x, SLOT), :], z_send, z_recv, (gr, f, tp))

        loop(0, n_fs - 1, back)
        ret[span(fs * per + x, SLOT), :] = summed[x, span(fs, SLOT), :]

    def serve(x):
        def twins(k):
            source = jnp.where(k > 0, other_from(k - 1), fs)
            index = gr * n_fs + source

            @pl.when((x == per - 1) & (k == n_fs - 1))
            def _():
                tell_sent()

            @pl.when(source != fs)
            def _():
                for w, out in enumerate((gate_land, up_land)):
                    settle(own_row(out, x, index), w_recv.at[w, x, source])

            for w, out in enumerate((gate_land, up_land)):
                place = own_row(out, x, index)
                for j in range(1, n_gr):
                    g = (gr + j) % n_gr
                    remote(place, place, twin_send.at[w, g], twin_recv.at[w, x, gr], (g, fs, tp))

            @pl.when(index // per_tp == tp)
            def _():
                place = own_row(down_land, x, index - tp * per_tp)

                @pl.when(source != fs)
                def _():
                    settle(place, w_recv.at[2, x, source])

                @pl.when(source == fs)
                def _():
                    if n_tp > 1:
                        settle(down_land.at[x, span(index - tp * per_tp, blk), pl.ds(0, (n_tp - 1) * wide)], w_recv.at[2, x, fs])

                for j in range(1, n_gr):
                    g = (gr + j) % n_gr
                    remote(place, place, twin_send.at[2, g], twin_recv.at[2, x, gr], (g, fs, tp))

        loop(0, n_fs, twins)
        for j in range(1, n_gr):
            g = (gr + j) % n_gr
            for w, out in enumerate((gate_land, up_land)):
                settle(out.at[x, span(g, n_fs * blk), :], twin_recv.at[w, x, g])

        @pl.when(home != gr)
        def _():
            settle(down_land.at[x], twin_recv.at[2, x, home])

        loads = [
            pltpu.make_async_copy(gate_land.at[x], w_vmem.at[0], load_sem.at[0]),
            pltpu.make_async_copy(up_land.at[x], w_vmem.at[1], load_sem.at[1]),
            pltpu.make_async_copy(down_land.at[x], down_vmem, load_sem.at[2]),
        ]
        for copy in loads:
            copy.start()
        @pl.when(x == per - 1)
        def _():
            pl.semaphore_wait(sent_sem, half - 1)
            loop(0, per - 1, give_back)

        loads[0].wait()
        loads[1].wait()

        def hide(c):
            cut = span(c, tile)
            gate_pre = dot(rows[x], w_vmem[0, :, cut])
            up_pre = dot(rows[x], w_vmem[1, :, cut])
            hidden[:, cut] = (jax.nn.silu(gate_pre) * up_pre).astype(BF16)

        loop(0, wide // tile, hide)
        loads[2].wait()

        def lower(c):
            cut = span(c, tile_full)
            part[x, :, cut] = dot(hidden[...], down_vmem[:, cut]).astype(BF16)

        loop(0, full // tile_full, lower)
        for j in range(1, n_tp):
            t = (tp + j) % n_tp
            remote(part.at[x, :, span(t, wide)], got.at[tp, x], x_send.at[t], x_recv.at[tp, x], (gr, fs, t))
        for j in range(1, n_tp):
            t = (tp + j) % n_tp
            settle(got.at[t, x], x_recv.at[t, x])

        def add(f):
            total = part[x, span(f, SLOT), span(tp, wide)].astype(F32)
            for j in range(1, n_tp):
                total = total + got[(tp + j) % n_tp, x, span(f, SLOT), :].astype(F32)
            summed[x, span(f, SLOT), :] = total.astype(BF16)

        loop(0, n_fs, add)

        @pl.when(x == per - 1)
        def _():
            give_back(x)

    loop(0, per, serve)

    settle(ret.at[pl.ds(0, (n_fs - 1) * per * SLOT)], z_recv)

    def mix(c):
        cut = span(c, tile)
        total = sum(
            lax.dot_general(pick[j], ret[:, cut], (((0,), (0,)), ((), ())), preferred_element_type=F32)
            for j in range(2)
        )
        mixed[:, cut] = total[0:toks].astype(BF16)

    loop(0, wide // tile, mix)

    settle(tok_own.at[pl.ds(0, groups - 1)], tok_send)
    settle(meta_land.at[pl.ds(0, n_fs - 1)], meta_send)

    def drain_share(q):
        for _ in range(reach * n_tp - 1):
            settle(tok_land.at[0, pl.ds(0, seats)], share_send)

    loop(0, 1, drain_share)
    for j in range(1, n_gr):
        g = (gr + j) % n_gr
        for w, out in enumerate((gate_land, up_land)):
            settle(out.at[:, span(gr, n_fs * blk), :], twin_send.at[w, g])

        @pl.when(home == gr)
        def _():
            settle(down_land, twin_send.at[2, g])

    for j in range(1, n_tp):
        t = (tp + j) % n_tp
        settle(part.at[:, :, span(t, wide)], x_send.at[t])
    settle(ret.at[pl.ds(0, (n_fs - 1) * per * SLOT)], z_send)


def copy_kernel(gate, up, down, mixed, gate_out, up_out, down_out, mixed_out):
    gate_out[...] = gate[...]
    up_out[...] = up[...]
    down_out[...] = down[...]
    mixed_out[...] = mixed[...]


def hand_over(gate, up, down, mixed):
    per = gate.shape[0]
    parts = 4

    def spec(array):
        return pl.BlockSpec((1, array.shape[1] // parts, array.shape[2]), lambda x, c: (x, c, 0))

    specs = [spec(gate), spec(up), spec(down), pl.BlockSpec(mixed.shape, lambda x, c: (0, 0))]
    return pl.pallas_call(
        copy_kernel,
        grid=(per, parts),
        out_shape=tuple(jax.ShapeDtypeStruct(a.shape, a.dtype) for a in (gate, up, down, mixed)),
        in_specs=specs,
        out_specs=tuple(specs),
        compiler_params=pltpu.CompilerParams(vmem_limit_bytes=60 * 1024 * 1024),
        name="hand_over",
    )(gate, up, down, mixed)


def body(sizes, prompt, norm_gain, gate_weight, up_weight, down_weight, routes, route_weight):
    n_gr, n_fs, n_tp = sizes
    tok_count, wide = prompt.shape
    full = wide * n_tp
    experts, blk, _ = gate_weight.shape
    per = experts // n_fs
    groups = experts // EXP_GROUP
    reach = EXP_GROUP // per
    seats = n_fs // reach
    rows_all = n_gr * n_fs * blk
    pad = -(-tok_count // 128) * 128
    any_spec = pl.BlockSpec(memory_space=pl.ANY)
    vmem_spec = pl.BlockSpec(memory_space=pltpu.VMEM)
    dma = pltpu.SemaphoreType.DMA
    held = n_fs * SLOT
    gate_land, up_land, down_land, _, mixed = pl.pallas_call(
        functools.partial(serve_kernel, sizes),
        out_shape=(
            jax.ShapeDtypeStruct((per, rows_all, wide), BF16),
            jax.ShapeDtypeStruct((per, rows_all, wide), BF16),
            jax.ShapeDtypeStruct((per, rows_all // n_tp, full), BF16),
            jax.ShapeDtypeStruct((3, experts, blk, wide), BF16),
            jax.ShapeDtypeStruct((tok_count, wide), BF16),
        ),
        in_specs=[any_spec] * 3 + [vmem_spec] * 4,
        out_specs=(any_spec,) * 4 + (vmem_spec,),
        scratch_shapes=[
            pltpu.VMEM((IN_SLOTS, 3, blk, wide), F32),
            pltpu.VMEM((OUT_SLOTS, 3, blk, wide), BF16),
            pltpu.VMEM((pad, wide), BF16),
            pltpu.VMEM((8, pad), jnp.int32),
            pltpu.VMEM((8, pad), F32),
            pltpu.VMEM((groups, GROUP_ROWS, wide), BF16),
            pltpu.VMEM((groups, EXP_GROUP, GROUP_ROWS), F32),
            pltpu.VMEM((n_tp, n_fs, GROUP_ROWS, wide), BF16),
            pltpu.VMEM((n_fs, EXP_GROUP, GROUP_ROWS), F32),
            pltpu.VMEM((per, held, full), BF16),
            pltpu.VMEM((2, experts * SLOT, pad), BF16),
            pltpu.VMEM((2, rows_all, wide), BF16),
            pltpu.VMEM((rows_all // n_tp, full), BF16),
            pltpu.VMEM((held, wide), BF16),
            pltpu.VMEM((per, held, full), BF16),
            pltpu.VMEM((n_tp, per, held, wide), BF16),
            pltpu.VMEM((per, held, wide), BF16),
            pltpu.VMEM((experts * SLOT, wide), BF16),
            dma((IN_SLOTS, 3)),
            dma((OUT_SLOTS, 3)),
            dma((3,)),
            dma((3, per, n_fs)),
            dma(()),
            dma((seats,)),
            dma(()),
            dma((n_tp,)),
            dma(()),
            dma(()),
            dma((3, n_gr)),
            dma((3, per, n_gr)),
            dma((3,)),
            dma((n_tp,)),
            dma((n_tp, per)),
            dma(()),
            dma(()),
            pltpu.SemaphoreType.REGULAR,
        ],
        compiler_params=pltpu.CompilerParams(
            collective_id=0, has_side_effects=True, vmem_limit_bytes=58 * 1024 * 1024
        ),
        name="serve",
    )(gate_weight, up_weight, down_weight, norm_gain.reshape(1, blk), prompt, routes.T, route_weight.T)
    return hand_over(gate_land, up_land, down_land, mixed)


def solution(mesh):
    sizes = (mesh.shape["gr"], mesh.shape["fs"], mesh.shape["tp"])
    return jax.shard_map(
        functools.partial(body, sizes),
        mesh=mesh,
        in_specs=(
            P(("gr", "fs"), "tp"),
            P(("gr", "fs")),
            P(None, ("gr", "fs"), "tp"),
            P(None, ("gr", "fs"), "tp"),
            P(None, ("gr", "fs"), "tp"),
            P(("gr", "fs"), None),
            P(("gr", "fs"), None),
        ),
        out_specs=(
            P("fs", None, "tp"),
            P("fs", None, "tp"),
            P("fs", "tp", None),
            P(("gr", "fs"), "tp"),
        ),
        check_vma=False,
    )
```

```python
import functools

import jax
import jax.numpy as jnp
from jax import lax
from jax.experimental import pallas as pl
from jax.experimental.pallas import tpu as pltpu
from jax.sharding import PartitionSpec as P

CAP = 30
EXP_GROUP = 8
SLOT = -(-CAP // 16) * 16
GROUP_ROWS = -(-(EXP_GROUP * CAP // 2) // 128) * 128
MESH = pl.DeviceIdType.MESH
F32, BF16 = jnp.float32, jnp.bfloat16


def remote(src, dst, send, recv, device):
    copy = pltpu.make_async_remote_copy(
        src_ref=src, dst_ref=dst, send_sem=send, recv_sem=recv, device_id=device, device_id_type=MESH
    )
    copy.start()


def settle(ref, sem):
    pltpu.make_async_copy(ref, ref, sem).wait()


def loop(low, high, step):
    lax.fori_loop(low, high, lambda index, carry: (step(index), carry)[1], 0)


def span(index, size):
    return pl.ds(pl.multiple_of(index * size, size), size)


def greet(barrier, device):
    pl.semaphore_signal(barrier, inc=1, device_id=device, device_id_type=MESH)


def iota(shape, axis):
    return lax.broadcasted_iota(jnp.int32, shape, axis)


def dot(a, b):
    return jnp.dot(a, b, preferred_element_type=F32)


IN_SLOTS = 3
OUT_SLOTS = 2
EARLY = 4


def serve_kernel(
    sizes, gate, up, down, gain, prompt, routes, shares,
    pair_land, down_land, cast, mixed,
    stage_in, stage_out, prompt_pad, routes_pad, shares_pad, tok_own, meta_own, tok_land, meta_land,
    rows, pick, w_vmem, down_vmem, hidden, part, got, summed, ret,
    in_sem, out_sem, w_send, w_recv, tok_send, tok_recv, share_send, share_recv,
    meta_send, meta_recv, twin_send, twin_recv, load_sem, x_send, x_recv, z_send, z_recv, sent_sem,
):
    n_gr, n_fs, n_tp = sizes
    gr, fs, tp = lax.axis_index("gr"), lax.axis_index("fs"), lax.axis_index("tp")
    experts, blk, wide = gate.shape
    per = experts // n_fs
    groups = experts // EXP_GROUP
    reach = EXP_GROUP // per
    seats = n_fs // reach
    full = wide * n_tp
    toks, pad = prompt.shape[0], prompt_pad.shape[0]
    per_tp = n_gr * n_fs // n_tp
    row = gr * n_fs + fs
    owner = row // per_tp
    home = tp * per_tp // n_fs
    ring = n_fs * n_tp
    steps = per * n_fs
    weights = (gate, up, down)
    gate_land, up_land = pair_land.at[:, 0], pair_land.at[:, 1]
    member = fs % reach
    my_group = fs // reach

    half = n_fs // 2
    base, local = fs // half * half, fs % half
    across = half - base
    blocks = per * (half - 1) // 3
    late = per * half - 2 * blocks
    odd = per * (half - 1) - 3 * blocks

    def plan(step):
        part, rest = step % 5, step - 5 * blocks
        early_far = step // 5 * 2 + jnp.where(part == 3, 1, 0)
        early_near = step // 5 * 3 + jnp.where(part == 4, 2, jnp.where(part == 2, 1, 0))
        in_early = step < 5 * blocks
        is_far = jnp.where(in_early, (part == 0) | (part == 3), rest < late)
        is_own = step >= 5 * blocks + late + odd
        far = jnp.where(in_early, early_far, 2 * blocks + rest)
        near = jnp.where(in_early, early_near, 3 * blocks + rest - late)
        far_x, far_f = far // half, across + (local + half - 1 - far % half) % half
        near_x = near // max(half - 1, 1)
        near_f = base + (local + 1 + near % max(half - 1, 1)) % half
        x = jnp.where(is_own, rest - late - odd, jnp.where(is_far, far_x, near_x))
        return x, jnp.where(is_own, fs, jnp.where(is_far, far_f, near_f))

    def other_to(k):
        return jnp.where(k < half - 1, base + (local + 1 + k) % half, across + (local + k + 1 - half) % half)

    def other_from(k):
        near = base + (local + 2 * half - 1 - k) % half
        return jnp.where(k < half - 1, near, across + (local + 2 * half - 1 - k) % half)

    def load(step):
        x, f = plan(step)
        e = f * per + x
        slot = step % IN_SLOTS
        return [
            pltpu.make_async_copy(ref.at[e], stage_in.at[slot, w], in_sem.at[slot, w])
            for w, ref in enumerate(weights)
        ]

    def start_load(step):
        for copy in load(step):
            copy.start()

    for step in range(min(IN_SLOTS, steps)):
        start_load(step)

    barrier = pltpu.get_barrier_semaphore()

    def greet_plane(k):
        other = (fs * n_tp + tp + k) % ring
        greet(barrier, (gr, other // n_tp, other % n_tp))

    loop(1, ring, greet_plane)
    loop(1, n_gr, lambda k: greet(barrier, ((gr + k) % n_gr, fs, tp)))
    def own_row(out, x, index):
        return out.at[x, span(index, blk), :]

    def pair_row(x, index):
        return pair_land.at[x, :, span(index, blk), :]

    def down_place(x, index, t):
        return down_land.at[x, span(index, blk), span(t, wide)]

    square = iota((blk, blk), 0) == iota((blk, blk), 1)
    scale = jnp.sum(jnp.where(square, gain[...], 0.0), axis=1, keepdims=True)

    def put(step):
        (x, f), slot = plan(step), step % OUT_SLOTS
        e = f * per + x

        @pl.when(f != fs)
        def _():
            for w in range(3):
                pltpu.make_async_copy(stage_out.at[slot, w], cast.at[e, w], out_sem.at[slot, w]).start()

        @pl.when(f == fs)
        def _():
            for w, out in enumerate((gate_land, up_land)):
                pltpu.make_async_copy(stage_out.at[slot, w], own_row(out, x, row), out_sem.at[slot, w]).start()

            @pl.when(owner == tp)
            def _():
                place = down_place(x, row - owner * per_tp, tp)
                pltpu.make_async_copy(stage_out.at[slot, 2], place, out_sem.at[slot, 2]).start()

            @pl.when(owner != tp)
            def _():
                pltpu.make_async_copy(stage_out.at[slot, 2], cast.at[e, 2], out_sem.at[slot, 2]).start()

    def dispatch(step):
        (x, f), slot = plan(step), step % OUT_SLOTS
        e = f * per + x
        for w in range(3):
            settle(stage_out.at[slot, w], out_sem.at[slot, w])

        @pl.when(f != fs)
        def _():
            pair = cast.at[e, pl.ds(0, 2)]
            remote(pair, pair_row(x, row), w_send.at[0], w_recv.at[0, x, fs], (gr, f, tp))
            place = down_place(x, row - owner * per_tp, tp)
            remote(cast.at[e, 2], place, w_send.at[2], w_recv.at[2, x, fs], (gr, f, owner))

        @pl.when((f == fs) & (owner != tp))
        def _():
            place = down_place(x, row - owner * per_tp, tp)
            remote(cast.at[e, 2], place, w_send.at[2], w_recv.at[2, x, fs], (gr, fs, owner))

    def convert(step):
        slot, out_slot = step % IN_SLOTS, step % OUT_SLOTS
        for copy in load(step):
            copy.wait()
        stage_out[out_slot, 0] = (stage_in[slot, 0] * scale).astype(BF16)
        stage_out[out_slot, 1] = (stage_in[slot, 1] * scale).astype(BF16)
        stage_out[out_slot, 2] = stage_in[slot, 2].astype(BF16)
        put(step)

        @pl.when(step + IN_SLOTS < steps)
        def _():
            start_load(step + IN_SLOTS)

    def cast_step(step):
        convert(step)
        dispatch(step - 1)

    early = min(EARLY, steps)
    convert(jnp.int32(0))
    pl.semaphore_wait(barrier, ring + n_gr - 2)
    loop(1, early, cast_step)

    prompt_pad[pl.ds(0, toks), :] = prompt[...]
    if pad > toks:
        prompt_pad[pl.ds(toks, pad - toks), :] = jnp.zeros((pad - toks, wide), BF16)
    routes_pad[...] = jnp.full(routes_pad.shape, -1, jnp.int32)
    routes_pad[0:2, 0:toks] = routes[...]
    shares_pad[...] = jnp.zeros(shares_pad.shape, F32)
    shares_pad[0:2, 0:toks] = shares[...]
    first, second = routes_pad[0:1, :], routes_pad[1:2, :]
    group_pad = -(-groups // 8) * 8
    low = iota((group_pad, pad), 0) * EXP_GROUP
    in_group = (first >= low) & (first < low + EXP_GROUP)
    expert_ids = iota((experts, pad), 0)
    named = (first == expert_ids) | (second == expert_ids)
    before = jnp.where(iota((pad, pad), 0) < iota((pad, pad), 1), 1.0, 0.0).astype(BF16)
    place_in = dot(jnp.where(in_group, 1.0, 0.0).astype(BF16), before).astype(jnp.int32)
    slot_raw = dot(jnp.where(named, 1.0, 0.0).astype(BF16), before)
    slot_in = jnp.where(named, slot_raw + 1.0, 0.0).astype(BF16)
    spots = []
    for r in (first, second):
        slot_of = jnp.sum(jnp.where(r == expert_ids, slot_raw, 0.0), axis=0, keepdims=True)
        spots.append(r * SLOT + slot_of.astype(jnp.int32))
    place_in = jnp.where(in_group, place_in, -1)
    for g in range(groups):
        pack = jnp.where(iota((GROUP_ROWS, pad), 0) == place_in[g : g + 1, :], 1.0, 0.0).astype(BF16)
        tok_own[g] = dot(pack, prompt_pad[...]).astype(BF16)
        meta_own[g] = lax.dot_general(
            slot_in[g * EXP_GROUP : (g + 1) * EXP_GROUP, :], pack,
            (((1,), (1,)), ((), ())), preferred_element_type=F32,
        )

    def send_tok(k):
        g = (my_group + k) % groups
        f = g * reach + member
        remote(tok_own.at[g], tok_land.at[tp, fs], tok_send, tok_recv.at[fs // reach], (gr, f, tp))

    loop(1, groups, send_tok)
    tok_land[tp, fs] = tok_own[my_group]
    meta_land[fs] = meta_own[my_group]

    def send_meta(k):
        f = (fs + k) % n_fs
        remote(meta_own.at[f // reach], meta_land.at[fs], meta_send, meta_recv, (gr, f, tp))

    loop(1, n_fs, send_meta)

    loop(early, steps, cast_step)
    dispatch(jnp.int32(steps - 1))

    def share_tok(q):
        seat = (my_group + q) % seats
        source = seat * reach + member
        place = tok_land.at[tp, source]

        @pl.when(source != fs)
        def _():
            settle(place, tok_recv.at[seat])

        def forward(j):
            seat_of = (member * n_tp + tp + j) % (reach * n_tp)
            f, t = my_group * reach + seat_of // n_tp, seat_of % n_tp
            remote(place, place, share_send, share_recv.at[tp], (gr, f, t))

        loop(1, reach * n_tp, forward)

    loop(0, seats, share_tok)

    def place_picks(e):
        ids = iota((SLOT, pad), 0) + e * SLOT
        weight = jnp.where(ids == spots[0], shares_pad[0:1, :], 0.0) + jnp.where(ids == spots[1], shares_pad[1:2, :], 0.0)
        high = weight.astype(BF16)
        pick[0, span(e, SLOT), :] = high
        pick[1, span(e, SLOT), :] = (weight - high.astype(F32)).astype(BF16)

    loop(0, experts, place_picks)

    for j in range(n_tp):
        t = (tp + j) % n_tp
        if j > 0:
            settle(tok_land.at[t], share_recv.at[t])
        elif reach > 1:
            settle(tok_land.at[t, pl.ds(0, n_fs - seats)], share_recv.at[t])
    settle(meta_land.at[pl.ds(0, n_fs - 1)], meta_recv)

    def make_rows(source):
        total = jnp.zeros((GROUP_ROWS, 1), F32)
        for t in range(n_tp):
            values = tok_land[t, source].astype(F32)
            total = total + jnp.sum(values * values, axis=1, keepdims=True)
        factor = lax.rsqrt(total / full + 1e-06)
        for t in range(n_tp):
            normed = (tok_land[t, source].astype(F32) * factor).astype(BF16)
            for x in range(per):
                line = meta_land[source, pl.ds(member * per + x, 1), :]
                choose = jnp.where(
                    iota((SLOT, GROUP_ROWS), 0) + 1 == line.astype(jnp.int32), 1.0, 0.0
                ).astype(BF16)
                rows[x, span(source, SLOT), t * wide : (t + 1) * wide] = dot(choose, normed).astype(BF16)

    loop(0, n_fs, make_rows)

    tile = min(wide, 256)
    tile_full = min(full, 256)

    def tell_sent():
        settle(cast.at[pl.ds(0, (n_fs - 1) * per), pl.ds(0, 2)], w_send.at[0])

        @pl.when(owner == tp)
        def _():
            settle(cast.at[pl.ds(0, (n_fs - 1) * per), 2], w_send.at[2])

        @pl.when(owner != tp)
        def _():
            settle(cast.at[:, 2], w_send.at[2])

        loop(1, half, lambda k: greet(sent_sem, (gr, base + (local + k) % half, tp)))

    def give_back(x):
        def back(k):
            f = other_to(k)
            remote(summed.at[x, span(f, SLOT), :], ret.at[span(fs * per + x, SLOT), :], z_send, z_recv, (gr, f, tp))

        loop(0, n_fs - 1, back)
        ret[span(fs * per + x, SLOT), :] = summed[x, span(fs, SLOT), :]

    def serve(x):
        def twins(k):
            source = jnp.where(k > 0, other_from(k - 1), fs)
            index = gr * n_fs + source

            @pl.when((x == per - 1) & (k == n_fs - 1))
            def _():
                tell_sent()

            @pl.when(source != fs)
            def _():
                settle(pair_row(x, index), w_recv.at[0, x, source])

            place = pair_row(x, index)
            for j in range(1, n_gr):
                g = (gr + j) % n_gr
                remote(place, place, twin_send.at[0, g], twin_recv.at[0, x, gr], (g, fs, tp))

            @pl.when(index // per_tp == tp)
            def _():
                place = own_row(down_land, x, index - tp * per_tp)

                @pl.when(source != fs)
                def _():
                    settle(place, w_recv.at[2, x, source])

                @pl.when(source == fs)
                def _():
                    if n_tp > 1:
                        settle(down_land.at[x, span(index - tp * per_tp, blk), pl.ds(0, (n_tp - 1) * wide)], w_recv.at[2, x, fs])

                for j in range(1, n_gr):
                    g = (gr + j) % n_gr
                    remote(place, place, twin_send.at[2, g], twin_recv.at[2, x, gr], (g, fs, tp))

        loop(0, n_fs, twins)
        for j in range(1, n_gr):
            g = (gr + j) % n_gr
            settle(pair_land.at[x, :, span(g, n_fs * blk), :], twin_recv.at[0, x, g])

        @pl.when(home != gr)
        def _():
            settle(down_land.at[x], twin_recv.at[2, x, home])

        loads = [
            pltpu.make_async_copy(gate_land.at[x], w_vmem.at[0], load_sem.at[0]),
            pltpu.make_async_copy(up_land.at[x], w_vmem.at[1], load_sem.at[1]),
            pltpu.make_async_copy(down_land.at[x], down_vmem, load_sem.at[2]),
        ]
        for copy in loads:
            copy.start()
        @pl.when(x == per - 1)
        def _():
            pl.semaphore_wait(sent_sem, half - 1)
            loop(0, per - 1, give_back)

        loads[0].wait()
        loads[1].wait()

        def hide(c):
            cut = span(c, tile)
            gate_pre = dot(rows[x], w_vmem[0, :, cut])
            up_pre = dot(rows[x], w_vmem[1, :, cut])
            hidden[:, cut] = (jax.nn.silu(gate_pre) * up_pre).astype(BF16)

        loop(0, wide // tile, hide)
        loads[2].wait()

        def lower(c):
            cut = span(c, tile_full)
            part[x, :, cut] = dot(hidden[...], down_vmem[:, cut]).astype(BF16)

        loop(0, full // tile_full, lower)
        for j in range(1, n_tp):
            t = (tp + j) % n_tp
            remote(part.at[x, :, span(t, wide)], got.at[tp, x], x_send.at[t], x_recv.at[tp, x], (gr, fs, t))
        for j in range(1, n_tp):
            t = (tp + j) % n_tp
            settle(got.at[t, x], x_recv.at[t, x])

        def add(f):
            total = part[x, span(f, SLOT), span(tp, wide)].astype(F32)
            for j in range(1, n_tp):
                total = total + got[(tp + j) % n_tp, x, span(f, SLOT), :].astype(F32)
            summed[x, span(f, SLOT), :] = total.astype(BF16)

        loop(0, n_fs, add)

        @pl.when(x == per - 1)
        def _():
            give_back(x)

    loop(0, per, serve)

    settle(ret.at[pl.ds(0, (n_fs - 1) * per * SLOT)], z_recv)

    def mix(c):
        cut = span(c, tile)
        total = sum(
            lax.dot_general(pick[j], ret[:, cut], (((0,), (0,)), ((), ())), preferred_element_type=F32)
            for j in range(2)
        )
        mixed[:, cut] = total[0:toks].astype(BF16)

    loop(0, wide // tile, mix)

    settle(tok_own.at[pl.ds(0, groups - 1)], tok_send)
    settle(meta_land.at[pl.ds(0, n_fs - 1)], meta_send)

    def drain_share(q):
        for _ in range(reach * n_tp - 1):
            settle(tok_land.at[0, pl.ds(0, seats)], share_send)

    loop(0, 1, drain_share)
    for j in range(1, n_gr):
        g = (gr + j) % n_gr
        settle(pair_land.at[:, :, span(gr, n_fs * blk), :], twin_send.at[0, g])

        @pl.when(home == gr)
        def _():
            settle(down_land, twin_send.at[2, g])

    for j in range(1, n_tp):
        t = (tp + j) % n_tp
        settle(part.at[:, :, span(t, wide)], x_send.at[t])
    settle(ret.at[pl.ds(0, (n_fs - 1) * per * SLOT)], z_send)


def copy_kernel(pair, down, mixed, gate_out, up_out, down_out, mixed_out):
    gate_out[...] = pair[:, 0]
    up_out[...] = pair[:, 1]
    down_out[...] = down[...]
    mixed_out[...] = mixed[...]


def hand_over(pair, down, mixed):
    per, _, rows, wide = pair.shape
    parts = 4
    pair_spec = pl.BlockSpec((1, 2, rows // parts, wide), lambda x, c: (x, 0, c, 0))
    one_spec = pl.BlockSpec((1, rows // parts, wide), lambda x, c: (x, c, 0))
    down_spec = pl.BlockSpec((1, down.shape[1] // parts, down.shape[2]), lambda x, c: (x, c, 0))
    mixed_spec = pl.BlockSpec(mixed.shape, lambda x, c: (0, 0))
    one = jax.ShapeDtypeStruct((per, rows, wide), BF16)
    return pl.pallas_call(
        copy_kernel,
        grid=(per, parts),
        out_shape=(one, one, jax.ShapeDtypeStruct(down.shape, BF16), jax.ShapeDtypeStruct(mixed.shape, BF16)),
        in_specs=[pair_spec, down_spec, mixed_spec],
        out_specs=(one_spec, one_spec, down_spec, mixed_spec),
        compiler_params=pltpu.CompilerParams(vmem_limit_bytes=60 * 1024 * 1024),
        name="hand_over",
    )(pair, down, mixed)


def body(sizes, prompt, norm_gain, gate_weight, up_weight, down_weight, routes, route_weight):
    n_gr, n_fs, n_tp = sizes
    tok_count, wide = prompt.shape
    full = wide * n_tp
    experts, blk, _ = gate_weight.shape
    per = experts // n_fs
    groups = experts // EXP_GROUP
    reach = EXP_GROUP // per
    seats = n_fs // reach
    rows_all = n_gr * n_fs * blk
    pad = -(-tok_count // 128) * 128
    any_spec = pl.BlockSpec(memory_space=pl.ANY)
    vmem_spec = pl.BlockSpec(memory_space=pltpu.VMEM)
    dma = pltpu.SemaphoreType.DMA
    held = n_fs * SLOT
    pair_land, down_land, _, mixed = pl.pallas_call(
        functools.partial(serve_kernel, sizes),
        out_shape=(
            jax.ShapeDtypeStruct((per, 2, rows_all, wide), BF16),
            jax.ShapeDtypeStruct((per, rows_all // n_tp, full), BF16),
            jax.ShapeDtypeStruct((experts, 3, blk, wide), BF16),
            jax.ShapeDtypeStruct((tok_count, wide), BF16),
        ),
        in_specs=[any_spec] * 3 + [vmem_spec] * 4,
        out_specs=(any_spec,) * 3 + (vmem_spec,),
        scratch_shapes=[
            pltpu.VMEM((IN_SLOTS, 3, blk, wide), F32),
            pltpu.VMEM((OUT_SLOTS, 3, blk, wide), BF16),
            pltpu.VMEM((pad, wide), BF16),
            pltpu.VMEM((8, pad), jnp.int32),
            pltpu.VMEM((8, pad), F32),
            pltpu.VMEM((groups, GROUP_ROWS, wide), BF16),
            pltpu.VMEM((groups, EXP_GROUP, GROUP_ROWS), F32),
            pltpu.VMEM((n_tp, n_fs, GROUP_ROWS, wide), BF16),
            pltpu.VMEM((n_fs, EXP_GROUP, GROUP_ROWS), F32),
            pltpu.VMEM((per, held, full), BF16),
            pltpu.VMEM((2, experts * SLOT, pad), BF16),
            pltpu.VMEM((2, rows_all, wide), BF16),
            pltpu.VMEM((rows_all // n_tp, full), BF16),
            pltpu.VMEM((held, wide), BF16),
            pltpu.VMEM((per, held, full), BF16),
            pltpu.VMEM((n_tp, per, held, wide), BF16),
            pltpu.VMEM((per, held, wide), BF16),
            pltpu.VMEM((experts * SLOT, wide), BF16),
            dma((IN_SLOTS, 3)),
            dma((OUT_SLOTS, 3)),
            dma((3,)),
            dma((3, per, n_fs)),
            dma(()),
            dma((seats,)),
            dma(()),
            dma((n_tp,)),
            dma(()),
            dma(()),
            dma((3, n_gr)),
            dma((3, per, n_gr)),
            dma((3,)),
            dma((n_tp,)),
            dma((n_tp, per)),
            dma(()),
            dma(()),
            pltpu.SemaphoreType.REGULAR,
        ],
        compiler_params=pltpu.CompilerParams(
            collective_id=0, has_side_effects=True, vmem_limit_bytes=58 * 1024 * 1024
        ),
        name="serve",
    )(gate_weight, up_weight, down_weight, norm_gain.reshape(1, blk), prompt, routes.T, route_weight.T)
    return hand_over(pair_land, down_land, mixed)


def solution(mesh):
    sizes = (mesh.shape["gr"], mesh.shape["fs"], mesh.shape["tp"])
    return jax.shard_map(
        functools.partial(body, sizes),
        mesh=mesh,
        in_specs=(
            P(("gr", "fs"), "tp"),
            P(("gr", "fs")),
            P(None, ("gr", "fs"), "tp"),
            P(None, ("gr", "fs"), "tp"),
            P(None, ("gr", "fs"), "tp"),
            P(("gr", "fs"), None),
            P(("gr", "fs"), None),
        ),
        out_specs=(
            P("fs", None, "tp"),
            P("fs", None, "tp"),
            P("fs", "tp", None),
            P(("gr", "fs"), "tp"),
        ),
        check_vma=False,
    )
```
